32 devices in a mesh: sp: 4 (over z), tp: 8 (over y, x, core).
Axes of the slice: x: 2, y: 2, z: 4, core: 2. Of those that a mesh axis runs over, the one named last changes fastest.
Arguments:
- stream: bfloat16 [1024, 4096], P('sp', 'tp'), may hold values from -80 to 80
- norm_gain: bfloat16 [3, 4096], replicated, may hold values from 0.099609375 to 1.8984375
- value_weight: bfloat16 [3, 2048, 4096], P(None, 'tp'), may hold values from -0.09375 to 0.09375
- gate_weight: bfloat16 [3, 2048, 4096], P(None, 'tp'), may hold values from -0.09375 to 0.09375
- kernel: float32 [3, 31, 2048], P(None, None, 'tp'), may hold values from -8 to 8
- kernel_bias: float32 [3, 2048], P(None, 'tp'), may hold values from -3 to 3
- chan_gain: float32 [3, 2048], P(None, 'tp'), may hold values from 0.1 to 1.9
- chan_shift: float32 [3, 2048], P(None, 'tp'), may hold values from -3 to 3
- out_weight: bfloat16 [3, 2048, 4096], P(None, None, 'tp'), may hold values from -0.125 to 0.125
Outputs:
- result: bfloat16 [1024, 4096], P('sp', 'tp')
The draws below stay inside these ranges and needn't reach their ends.
All inputs are finite; a program needn't handle non-finite values.
Results may differ from the reference program's by a relative error of at most 0.012.
Values may be sent and summed in bfloat16 or wider, within the bound.
A program may use at most 64 MiB of HBM per device.

```python
import jax
import jax.numpy as jnp
from jax import lax

D = 4096
DC = 2048
KW = 31
LAYERS = 3
TOKENS = 1024


def draw_stream(key, part):
    keys = jax.random.split(jax.random.fold_in(key, 11), 3)
    noise = jnp.clip(jax.random.normal(keys[0], (TOKENS, D), jnp.float32), -4.0, 4.0)
    column_scale = jnp.exp(jnp.log(3.0) * jnp.arange(D, dtype=jnp.float32) / D + jax.random.uniform(keys[1], (D,), jnp.float32, -0.8, 0.8))
    row_scale = jnp.exp(jax.random.uniform(keys[2], (TOKENS, 1), jnp.float32, jnp.log(0.3), jnp.log(3.0)))
    return (noise * column_scale[None, :] * row_scale).astype(jnp.bfloat16)


def draw_kernel(key, part):
    keys = jax.random.split(jax.random.fold_in(key, 23), 2)
    noise = jnp.clip(jax.random.normal(keys[0], (LAYERS, KW, DC), jnp.float32), -4.0, 4.0)
    channel_scale = jnp.exp(jnp.log(6.0) * jnp.arange(DC, dtype=jnp.float32) / DC + jax.random.uniform(keys[1], (LAYERS, 1, DC), jnp.float32, -0.5, 0.5))
    return noise * channel_scale / jnp.sqrt(1.0 * KW)


def levels(stream_key, extent, cuts, low, largest):
    loudness, own = 1.0, jax.random.fold_in(stream_key, 6)
    for position, shards_of in cuts:
        steps = jnp.exp(jax.random.uniform(jax.random.fold_in(own, position), (shards_of,), jnp.float32, low / len(cuts), largest / len(cuts)))
        loudness = loudness * jnp.repeat(steps, extent[position] // shards_of).reshape([-1 if axis == position else 1 for axis in range(len(extent))])
    return loudness


def normal_values(stream_key, extent, width, most, shards=(), held_as=jnp.bfloat16):
    loudness = levels(stream_key, extent, shards, -0.22, 0.18) if shards else 1.0
    drawn = jax.random.normal(stream_key, extent, jnp.float32) * width * loudness
    return jnp.minimum(jnp.maximum(drawn, -most), most).astype(held_as)


def setup_inputs(seed: int = 0) -> dict:
    key_of = jax.random.split(jax.random.key(seed), 10)
    stream = draw_stream(jax.random.fold_in(key_of[9], 71), 0)
    norm_gain = jnp.clip(1.0 + 0.18 * jax.random.normal(key_of[1], (LAYERS, D), jnp.float32), 0.099609375, 1.8984375).astype(jnp.bfloat16)
    value_weight = normal_values(key_of[2], (LAYERS, DC, D), D ** -0.5, 0.09375, ((1, 8),))
    gate_weight = normal_values(key_of[3], (LAYERS, DC, D), D ** -0.5, 0.09375, ((1, 8),))
    kernel = draw_kernel(jax.random.fold_in(key_of[9], 71), 0)
    kernel_bias = normal_values(key_of[5], (LAYERS, DC), 0.5, 3.0, ((1, 8),), jnp.float32)
    chan_gain = jnp.clip(1.0 + 0.18 * jax.random.normal(key_of[6], (LAYERS, DC), jnp.float32), 0.1, 1.9)
    chan_shift = normal_values(key_of[7], (LAYERS, DC), 0.5, 3.0, ((1, 8),), jnp.float32)
    out_weight = normal_values(key_of[8], (LAYERS, DC, D), DC ** -0.5, 0.125, ((2, 8),))
    return {"stream": stream, "norm_gain": norm_gain, "value_weight": value_weight, "gate_weight": gate_weight, "kernel": kernel, "kernel_bias": kernel_bias, "chan_gain": chan_gain, "chan_shift": chan_shift, "out_weight": out_weight}


EPSILON = 1e-06

def against(left, right):
    return lax.dot_general(left, right, (((1,), (1,)), ((), ())), preferred_element_type=jnp.float32)

def reference(stream, norm_gain, value_weight, gate_weight, kernel, kernel_bias, chan_gain, chan_shift, out_weight):
    current = stream
    for layer_at in range(LAYERS):
        wide_rows = current.astype(jnp.float32)
        scale_row = lax.rsqrt(lax.optimization_barrier(jnp.mean(wide_rows * wide_rows, axis=1, keepdims=True)) + EPSILON)
        normed = (wide_rows * scale_row * norm_gain[layer_at].astype(jnp.float32)[None, :]).astype(jnp.bfloat16)
        value_part = against(normed, value_weight[layer_at])
        gate_part = against(normed, gate_weight[layer_at])
        gated_rows = (value_part * jax.nn.sigmoid(gate_part)).astype(jnp.bfloat16)
        padded = jnp.pad(gated_rows.astype(jnp.float32), ((KW - 1, 0), (0, 0)))
        convolved = jnp.broadcast_to(kernel_bias[layer_at][None, :], (TOKENS, DC))
        for tap_at in range(KW):
            convolved = convolved + kernel[layer_at, tap_at][None, :] * padded[tap_at:tap_at + TOKENS]
        centre = lax.optimization_barrier(jnp.mean(convolved, axis=1, keepdims=True))
        spread = lax.optimization_barrier(jnp.mean(convolved * convolved, axis=1, keepdims=True)) - centre * centre
        normal_out = (convolved - centre) * lax.rsqrt(spread + EPSILON) * chan_gain[layer_at][None, :] + chan_shift[layer_at][None, :]
        hidden = jax.nn.silu(normal_out).astype(jnp.bfloat16)
        projected = jnp.dot(hidden, out_weight[layer_at], preferred_element_type=jnp.float32)
        current = (current.astype(jnp.float32) + projected).astype(jnp.bfloat16)
    return current
```

```python
import functools

import jax
import jax.numpy as jnp
from jax import lax
from jax.experimental import pallas as pl
from jax.experimental.pallas import tpu as pltpu
from jax.sharding import PartitionSpec as P

EPSILON = 1e-06


def passed_along(shard, axis, by):
    count = lax.axis_size(axis)
    pairs = [(i, i + by) for i in range(count) if 0 <= i + by < count]
    return lax.ppermute(shard, axis, pairs)


def against(left, right):
    return lax.dot_general(
        left, right, (((1,), (1,)), ((), ())), preferred_element_type=jnp.float32
    )


def on_device(
    stream,
    norm_gain,
    value_weight,
    gate_weight,
    kernel,
    kernel_bias,
    chan_gain,
    chan_shift,
    out_weight,
):
    layer_count = kernel.shape[0]
    reach_back = kernel.shape[1] - 1
    local_width = stream.shape[1]
    channels = kernel.shape[2] * lax.axis_size("tp")
    current = stream
    for layer_at in range(layer_count):
        gain_row = norm_gain[layer_at].astype(jnp.float32)
        value_matrix = value_weight[layer_at]
        gate_matrix = gate_weight[layer_at]
        row_count = current.shape[0]
        whole_rows = lax.all_gather(current, "tp", axis=1, tiled=True)
        whole_float = whole_rows.astype(jnp.float32)
        scale_row = lax.rsqrt(jnp.mean(whole_float * whole_float, axis=1, keepdims=True) + EPSILON)
        normed = (whole_float * scale_row * gain_row[None, :]).astype(jnp.bfloat16)
        value_part = against(normed, value_matrix)
        gate_part = against(normed, gate_matrix)
        gated_rows = (value_part * jax.nn.sigmoid(gate_part)).astype(jnp.bfloat16)
        earlier_taps = passed_along(gated_rows[row_count - reach_back :], "sp", 1)
        padded = jnp.concatenate([earlier_taps, gated_rows], axis=0)
        out_rows = padded.shape[0] - reach_back
        kernel_now = kernel[layer_at]
        convolved = jnp.broadcast_to(
            kernel_bias[layer_at][None, :], (out_rows, kernel_now.shape[1])
        )
        for tap_at in range(reach_back + 1):
            convolved = convolved + kernel_now[tap_at][None, :] * padded[
                tap_at : tap_at + out_rows
            ].astype(jnp.float32)
        totals = lax.psum(
            (jnp.sum(convolved, axis=1), jnp.sum(convolved * convolved, axis=1)), "tp"
        )
        centre = totals[0] / channels
        spread = totals[1] / channels - centre * centre
        normal_out = (convolved - centre[:, None]) * lax.rsqrt(spread + EPSILON)[
            :, None
        ] * chan_gain[layer_at][None, :] + chan_shift[layer_at][None, :]
        hidden = jax.nn.silu(normal_out).astype(jnp.bfloat16)
        out_matrix = out_weight[layer_at]

        def project_out(running, block_in, offset_at, out_matrix=out_matrix):
            return jnp.dot(block_in, out_matrix, preferred_element_type=jnp.float32)

        projected = project_out(
            jnp.zeros((out_rows, local_width), jnp.float32),
            lax.all_gather(hidden, "tp", axis=1, tiled=True),
            jnp.int32(0),
        )
        current = (current.astype(jnp.float32) + projected).astype(jnp.bfloat16)
    return current


LANES = 128
SUBLANES = 8
MESH = pl.DeviceIdType.MESH


def flipped(index, bit):
    return index + bit - 2 * bit * ((index // bit) % 2)


def fused_kernel(
    sp_count,
    tp_count,
    stream_ref,
    gain_ref,
    value_ref,
    gate_ref,
    kernel_ref,
    bias_ref,
    chan_gain_ref,
    chan_shift_ref,
    out_weight_ref,
    result_ref,
    cur_buf,
    hid_buf,
    weights,
    out_weights,
    gain32,
    acc,
    squares,
    padded,
    conv,
    gated_buf,
    halo,
    stat_buf,
    cur_recv,
    cur_send,
    hid_recv,
    hid_send,
    stat_recv,
    stat_send,
    halo_recv,
    halo_send,
    weight_sem,
    stream_sem,
):
    sp = lax.axis_index("sp")
    me = lax.axis_index("tp")
    layers, taps, local_channels = kernel_ref.shape
    rows, local_width = stream_ref.shape
    width = local_width * tp_count
    channels = local_channels * tp_count
    half = rows // 2
    halo_rows = halo.shape[1]
    skip = halo_rows - (taps - 1)
    pc, px, py = flipped(me, 1), flipped(me, 2), flipped(me, 4)
    diag = flipped(px, 4)

    def weight_copies(layer):
        return (
            pltpu.make_async_copy(
                value_ref.at[layer],
                weights.at[layer, pl.ds(0, local_channels)],
                weight_sem.at[0, layer],
            ),
            pltpu.make_async_copy(
                gate_ref.at[layer],
                weights.at[layer, pl.ds(local_channels, local_channels)],
                weight_sem.at[1, layer],
            ),
            pltpu.make_async_copy(
                out_weight_ref.at[layer], out_weights.at[layer], weight_sem.at[2, layer]
            ),
        )

    own_copy = pltpu.make_async_copy(stream_ref, cur_buf.at[me], stream_sem)
    own_copy.start()
    for layer in range(layers):
        for copy in weight_copies(layer):
            copy.start()

    barrier = pltpu.get_barrier_semaphore()
    for ahead in range(1, tp_count):
        pl.semaphore_signal(
            barrier,
            inc=1,
            device_id=(sp, lax.rem(me + ahead, tp_count)),
            device_id_type=MESH,
        )

    around = (1, sp_count - 1) if sp_count > 1 else ()
    for ahead in around:
        pl.semaphore_signal(
            barrier,
            inc=1,
            device_id=(lax.rem(sp + ahead, sp_count), me),
            device_id_type=MESH,
        )

    for layer in range(layers):
        gain32[layer] = gain_ref[layer : layer + 1].astype(jnp.float32)
    own_copy.wait()
    pl.semaphore_wait(barrier, tp_count - 1 + len(around))

    def gather(buf, send, recv, consume):
        def copy(slot, part, to, at):
            piece = buf.at[slot, pl.ds(part * half, half)]
            return pltpu.make_async_remote_copy(
                src_ref=piece,
                dst_ref=piece,
                send_sem=send.at[at],
                recv_sem=recv.at[slot, part],
                device_id=(sp, to),
                device_id_type=MESH,
            )

        started = []

        def go(slot, part, to):
            one = copy(slot, part, to, len(started))
            one.start()
            started.append(one)

        def arrived(slot, part):
            copy(slot, part, pc, 0).wait_recv()

        go(me, 0, px)
        go(me, 1, py)
        go(me, 1, px)
        go(me, 0, py)
        go(me, 0, pc)
        go(me, 1, pc)
        consume(me, True)
        arrived(pc, 0)
        arrived(pc, 1)
        consume(pc, False)
        arrived(px, 0)
        go(px, 0, py)
        go(px, 0, pc)
        arrived(py, 1)
        go(py, 1, px)
        go(py, 1, pc)
        arrived(px, 1)
        go(px, 1, pc)
        arrived(py, 0)
        go(py, 0, pc)
        consume(px, False)
        consume(py, False)
        for slot in (flipped(pc, 2), flipped(pc, 4)):
            arrived(slot, 0)
            arrived(slot, 1)
            consume(slot, False)
        arrived(diag, 0)
        go(diag, 0, pc)
        arrived(diag, 1)
        go(diag, 1, pc)
        consume(diag, False)
        last = flipped(diag, 1)
        arrived(last, 0)
        arrived(last, 1)
        consume(last, False)
        for one in started:
            one.wait_send()

    def row(ref, layer):
        picked = ref[0:1]
        for at in range(1, layers):
            picked = jnp.where(layer == at, ref[at : at + 1], picked)
        return picked

    def one_layer(layer, carry):
        value_copy, gate_copy, out_copy = weight_copies(layer)
        value_copy.wait()
        gate_copy.wait()

        def consume_current(slot, first):
            at = pl.multiple_of(slot * local_width, LANES)
            block = cur_buf[slot].astype(jnp.float32)
            squared = block * block
            partial = squared[:, :LANES]
            for lane in range(LANES, local_width, LANES):
                partial = partial + squared[:, lane : lane + LANES]
            gained = (block * gain32[layer, :, pl.ds(at, local_width)]).astype(jnp.bfloat16)
            product = against(gained, weights[layer, :, pl.ds(at, local_width)])
            if first:
                squares[...] = partial
                acc[...] = product
            else:
                squares[...] += partial
                acc[...] += product

        gather(cur_buf, cur_send, cur_recv, consume_current)

        scale = lax.rsqrt(jnp.sum(squares[...], axis=1, keepdims=True) / width + EPSILON)
        gated = (
            acc[:, :local_channels]
            * scale
            * jax.nn.sigmoid(acc[:, local_channels:] * scale)
        ).astype(jnp.bfloat16)
        gated_buf[...] = gated[rows - halo_rows :]

        def halo_copy(to):
            return pltpu.make_async_remote_copy(
                src_ref=gated_buf,
                dst_ref=halo.at[layer],
                send_sem=halo_send,
                recv_sem=halo_recv.at[layer],
                device_id=(to, me),
                device_id_type=MESH,
            )

        @pl.when(sp < sp_count - 1)
        def _():
            halo_copy(sp + 1).start()

        padded[pl.ds(halo_rows, rows)] = gated.astype(jnp.float32)

        @pl.when(sp == 0)
        def _():
            padded[pl.ds(0, halo_rows)] = jnp.zeros((halo_rows, local_channels), jnp.float32)

        tile = min(64, rows)
        bias = row(bias_ref, layer)

        def convolve(first_row):
            for lane in range(0, local_channels, LANES):
                total = jnp.broadcast_to(bias[:, lane : lane + LANES], (tile, LANES))
                for tap in range(taps):
                    total = total + kernel_ref[layer, tap : tap + 1, lane : lane + LANES] * padded[
                        first_row + skip + tap : first_row + skip + tap + tile, lane : lane + LANES
                    ]
                conv[first_row : first_row + tile, lane : lane + LANES] = total

        for first_row in range(tile, rows, tile):
            convolve(first_row)

        @pl.when(sp > 0)
        def _():
            halo_copy(sp - 1).wait_recv()
            padded[pl.ds(0, halo_rows)] = halo[layer].astype(jnp.float32)

        convolve(0)

        convolved = conv[...]
        lanes = lax.broadcasted_iota(jnp.int32, (rows, LANES), 1)
        total = jnp.sum(convolved, axis=1, keepdims=True)
        total_squared = jnp.sum(convolved * convolved, axis=1, keepdims=True)
        both = jnp.where(lanes == 0, total, jnp.where(lanes == 1, total_squared, 0.0))
        stat_buf[me] = both.T[:SUBLANES]

        def stat_copy(slot, to, at):
            return pltpu.make_async_remote_copy(
                src_ref=stat_buf.at[slot],
                dst_ref=stat_buf.at[slot],
                send_sem=stat_send.at[at],
                recv_sem=stat_recv.at[slot],
                device_id=(sp, to),
                device_id_type=MESH,
            )

        peers = [diag, flipped(diag, 1), px, py, flipped(px, 1), flipped(py, 1), pc]
        sent = [stat_copy(me, peer, at) for at, peer in enumerate(peers)]
        for one in sent:
            one.start()
        for peer in peers[::-1]:
            stat_copy(peer, peer, 0).wait_recv()
        summed = stat_buf[0]
        for slot in range(1, tp_count):
            summed = summed + stat_buf[slot]
        summed = jnp.concatenate(
            [summed, jnp.zeros((LANES - SUBLANES, rows), jnp.float32)], axis=0
        ).T
        centre = summed[:, 0:1] / channels
        spread = summed[:, 1:2] / channels - centre * centre
        normal_out = (convolved - centre) * lax.rsqrt(spread + EPSILON) * row(
            chan_gain_ref, layer
        ) + row(chan_shift_ref, layer)
        hid_buf[me] = (normal_out / (1.0 + jnp.exp(-normal_out))).astype(jnp.bfloat16)
        for one in sent:
            one.wait_send()

        @pl.when(sp < sp_count - 1)
        def _():
            halo_copy(sp + 1).wait_send()

        out_copy.wait()

        def consume_hidden(slot, first):
            at = pl.multiple_of(slot * local_channels, LANES)
            product = jnp.dot(
                hid_buf[slot],
                out_weights[layer, pl.ds(at, local_channels)],
                preferred_element_type=jnp.float32,
            )
            if first:
                acc[:, :local_width] = product
            else:
                acc[:, :local_width] += product

        gather(hid_buf, hid_send, hid_recv, consume_hidden)
        cur_buf[me] = (cur_buf[me].astype(jnp.float32) + acc[:, :local_width]).astype(jnp.bfloat16)
        return carry

    lax.fori_loop(0, layers, one_layer, 0)
    result_ref[...] = cur_buf[me]


def fused(
    sp_count,
    tp_count,
    stream,
    norm_gain,
    value_weight,
    gate_weight,
    kernel,
    kernel_bias,
    chan_gain,
    chan_shift,
    out_weight,
):
    layers, taps, local_channels = kernel.shape
    rows, local_width = stream.shape
    halo_rows = -(-(taps - 1) // 16) * 16
    any_space = pl.BlockSpec(memory_space=pl.ANY)
    vmem = pl.BlockSpec(memory_space=pltpu.VMEM)
    dma = pltpu.SemaphoreType.DMA
    return pl.pallas_call(
        functools.partial(fused_kernel, sp_count, tp_count),
        out_shape=jax.ShapeDtypeStruct((rows, local_width), jnp.bfloat16),
        in_specs=[any_space, vmem, any_space, any_space, vmem, vmem, vmem, vmem, any_space],
        out_specs=vmem,
        scratch_shapes=[
            pltpu.VMEM((tp_count, rows, local_width), jnp.bfloat16),
            pltpu.VMEM((tp_count, rows, local_channels), jnp.bfloat16),
            pltpu.VMEM((layers, 2 * local_channels, local_width * tp_count), jnp.bfloat16),
            pltpu.VMEM((layers,) + out_weight.shape[1:], jnp.bfloat16),
            pltpu.VMEM((layers, 1, local_width * tp_count), jnp.float32),
            pltpu.VMEM((rows, max(2 * local_channels, local_width)), jnp.float32),
            pltpu.VMEM((rows, LANES), jnp.float32),
            pltpu.VMEM((halo_rows + rows, local_channels), jnp.float32),
            pltpu.VMEM((rows, local_channels), jnp.float32),
            pltpu.VMEM((halo_rows, local_channels), jnp.bfloat16),
            pltpu.VMEM((layers, halo_rows, local_channels), jnp.bfloat16),
            pltpu.VMEM((tp_count, SUBLANES, rows), jnp.float32),
            dma((tp_count, 2)),
            dma((14,)),
            dma((tp_count, 2)),
            dma((14,)),
            dma((tp_count,)),
            dma((tp_count,)),
            dma((layers,)),
            dma,
            dma((3, layers)),
            dma,
        ],
        compiler_params=pltpu.CompilerParams(
            collective_id=0, has_side_effects=True, vmem_limit_bytes=60 * 1024 * 1024
        ),
    )(
        stream,
        norm_gain,
        value_weight,
        gate_weight,
        kernel,
        kernel_bias,
        chan_gain,
        chan_shift,
        out_weight,
    )


def solution(mesh):
    cube = mesh.shape["tp"] == 2**3
    body = functools.partial(fused, mesh.shape["sp"], mesh.shape["tp"]) if cube else on_device
    return jax.shard_map(
        body,
        mesh=mesh,
        in_specs=(
            P("sp", "tp"),
            P(),
            P(None, "tp", None),
            P(None, "tp", None),
            P(None, None, "tp"),
            P(None, "tp"),
            P(None, "tp"),
            P(None, "tp"),
            P(None, None, "tp"),
        ),
        out_specs=P("sp", "tp"),
        check_vma=False,
    )
```

```python
import functools

import jax
import jax.numpy as jnp
from jax import lax
from jax.experimental import pallas as pl
from jax.experimental.pallas import tpu as pltpu
from jax.sharding import PartitionSpec as P

EPSILON = 1e-06


def passed_along(shard, axis, by):
    count = lax.axis_size(axis)
    pairs = [(i, i + by) for i in range(count) if 0 <= i + by < count]
    return lax.ppermute(shard, axis, pairs)


def against(left, right):
    return lax.dot_general(
        left, right, (((1,), (1,)), ((), ())), preferred_element_type=jnp.float32
    )


def on_device(
    stream,
    norm_gain,
    value_weight,
    gate_weight,
    kernel,
    kernel_bias,
    chan_gain,
    chan_shift,
    out_weight,
):
    layer_count = kernel.shape[0]
    reach_back = kernel.shape[1] - 1
    local_width = stream.shape[1]
    channels = kernel.shape[2] * lax.axis_size("tp")
    current = stream
    for layer_at in range(layer_count):
        gain_row = norm_gain[layer_at].astype(jnp.float32)
        value_matrix = value_weight[layer_at]
        gate_matrix = gate_weight[layer_at]
        row_count = current.shape[0]
        whole_rows = lax.all_gather(current, "tp", axis=1, tiled=True)
        whole_float = whole_rows.astype(jnp.float32)
        scale_row = lax.rsqrt(jnp.mean(whole_float * whole_float, axis=1, keepdims=True) + EPSILON)
        normed = (whole_float * scale_row * gain_row[None, :]).astype(jnp.bfloat16)
        value_part = against(normed, value_matrix)
        gate_part = against(normed, gate_matrix)
        gated_rows = (value_part * jax.nn.sigmoid(gate_part)).astype(jnp.bfloat16)
        earlier_taps = passed_along(gated_rows[row_count - reach_back :], "sp", 1)
        padded = jnp.concatenate([earlier_taps, gated_rows], axis=0)
        out_rows = padded.shape[0] - reach_back
        kernel_now = kernel[layer_at]
        convolved = jnp.broadcast_to(
            kernel_bias[layer_at][None, :], (out_rows, kernel_now.shape[1])
        )
        for tap_at in range(reach_back + 1):
            convolved = convolved + kernel_now[tap_at][None, :] * padded[
                tap_at : tap_at + out_rows
            ].astype(jnp.float32)
        totals = lax.psum(
            (jnp.sum(convolved, axis=1), jnp.sum(convolved * convolved, axis=1)), "tp"
        )
        centre = totals[0] / channels
        spread = totals[1] / channels - centre * centre
        normal_out = (convolved - centre[:, None]) * lax.rsqrt(spread + EPSILON)[
            :, None
        ] * chan_gain[layer_at][None, :] + chan_shift[layer_at][None, :]
        hidden = jax.nn.silu(normal_out).astype(jnp.bfloat16)
        out_matrix = out_weight[layer_at]

        def project_out(running, block_in, offset_at, out_matrix=out_matrix):
            return jnp.dot(block_in, out_matrix, preferred_element_type=jnp.float32)

        projected = project_out(
            jnp.zeros((out_rows, local_width), jnp.float32),
            lax.all_gather(hidden, "tp", axis=1, tiled=True),
            jnp.int32(0),
        )
        current = (current.astype(jnp.float32) + projected).astype(jnp.bfloat16)
    return current


LANES = 128
SUBLANES = 8
MESH = pl.DeviceIdType.MESH


def flipped(index, bit):
    return index + bit - 2 * bit * ((index // bit) % 2)


def fused_kernel(
    sp_count,
    tp_count,
    stream_ref,
    gain_ref,
    value_ref,
    gate_ref,
    kernel_ref,
    bias_ref,
    chan_gain_ref,
    chan_shift_ref,
    out_weight_ref,
    result_ref,
    cur_buf,
    hid_buf,
    weights,
    out_weights,
    gain32,
    acc,
    squares,
    padded,
    conv,
    gated_buf,
    halo,
    stat_buf,
    par_buf,
    cur_recv,
    cur_send,
    hid_recv,
    hid_send,
    stat_recv,
    stat_send,
    par_recv,
    par_send,
    halo_recv,
    halo_send,
    weight_sem,
    stream_sem,
):
    sp = lax.axis_index("sp")
    me = lax.axis_index("tp")
    layers, taps, local_channels = kernel_ref.shape
    rows, local_width = stream_ref.shape
    width = local_width * tp_count
    channels = local_channels * tp_count
    half = rows // 2
    piece_rows = half // 2
    halo_rows = halo.shape[1]
    skip = halo_rows - (taps - 1)
    pc, px, py = flipped(me, 1), flipped(me, 2), flipped(me, 4)
    diag = flipped(px, 4)

    def weight_copies(layer):
        return (
            pltpu.make_async_copy(
                value_ref.at[layer],
                weights.at[layer, pl.ds(0, local_channels)],
                weight_sem.at[0, layer],
            ),
            pltpu.make_async_copy(
                gate_ref.at[layer],
                weights.at[layer, pl.ds(local_channels, local_channels)],
                weight_sem.at[1, layer],
            ),
            pltpu.make_async_copy(
                out_weight_ref.at[layer], out_weights.at[layer], weight_sem.at[2, layer]
            ),
        )

    own_copy = pltpu.make_async_copy(stream_ref, cur_buf.at[me], stream_sem)
    own_copy.start()
    for layer in range(layers):
        for copy in weight_copies(layer):
            copy.start()

    barrier = pltpu.get_barrier_semaphore()
    for ahead in range(1, tp_count):
        pl.semaphore_signal(
            barrier,
            inc=1,
            device_id=(sp, lax.rem(me + ahead, tp_count)),
            device_id_type=MESH,
        )

    around = (1, sp_count - 1) if sp_count > 1 else ()
    for ahead in around:
        pl.semaphore_signal(
            barrier,
            inc=1,
            device_id=(lax.rem(sp + ahead, sp_count), me),
            device_id_type=MESH,
        )

    for layer in range(layers):
        gain32[layer] = gain_ref[layer : layer + 1].astype(jnp.float32)
    own_copy.wait()
    pl.semaphore_wait(barrier, tp_count - 1 + len(around))

    peers = [diag, flipped(diag, 1), px, py, flipped(px, 1), flipped(py, 1), pc]

    def small_copies(buf, send, recv):
        def copy(slot, to, at):
            return pltpu.make_async_remote_copy(
                src_ref=buf.at[slot],
                dst_ref=buf.at[slot],
                send_sem=send.at[at],
                recv_sem=recv.at[slot],
                device_id=(sp, to),
                device_id_type=MESH,
            )

        sent = [copy(me, peer, at) for at, peer in enumerate(peers)]
        came = [copy(peer, peer, 0) for peer in peers[::-1]]
        return sent, came

    for layer in range(layers):
        par_buf[me, layer : layer + 1] = chan_gain_ref[layer : layer + 1]
        par_buf[me, layers + layer : layers + layer + 1] = chan_shift_ref[layer : layer + 1]

    class Gather:
        def __init__(self, buf, send, recv):
            self.buf, self.send, self.recv = buf, send, recv

        def copy(self, slot, part, to, at):
            piece = self.buf.at[slot, pl.ds(part * piece_rows, piece_rows)]
            return pltpu.make_async_remote_copy(
                src_ref=piece,
                dst_ref=piece,
                send_sem=self.send.at[at],
                recv_sem=self.recv.at[slot, part],
                device_id=(sp, to),
                device_id_type=MESH,
            )

        def first(self, h):
            self.copy(me, 2 * h, px, 14 * h).start()
            self.copy(me, 2 * h + 1, py, 14 * h + 1).start()
            self.copy(me, 2 * h, pc, 14 * h + 2).start()
            self.copy(me, 2 * h + 1, pc, 14 * h + 3).start()

        def second(self, h):
            self.copy(me, 2 * h + 1, px, 14 * h + 4).start()
            self.copy(me, 2 * h, py, 14 * h + 5).start()

        def arrived(self, slot, part):
            self.copy(slot, part, pc, 0).wait_recv()

        def half_arrived(self, slot, h):
            self.arrived(slot, 2 * h)
            self.arrived(slot, 2 * h + 1)

        def relay_first(self, h):
            self.arrived(px, 2 * h)
            self.copy(px, 2 * h, py, 14 * h + 6).start()
            self.copy(px, 2 * h, pc, 14 * h + 7).start()
            self.arrived(py, 2 * h + 1)
            self.copy(py, 2 * h + 1, px, 14 * h + 8).start()
            self.copy(py, 2 * h + 1, pc, 14 * h + 9).start()

        def relay_second(self, h):
            self.arrived(px, 2 * h + 1)
            self.copy(px, 2 * h + 1, pc, 14 * h + 10).start()
            self.arrived(py, 2 * h)
            self.copy(py, 2 * h, pc, 14 * h + 11).start()

        def relay_third(self, h):
            self.arrived(diag, 2 * h)
            self.copy(diag, 2 * h, pc, 14 * h + 12).start()
            self.arrived(diag, 2 * h + 1)
            self.copy(diag, 2 * h + 1, pc, 14 * h + 13).start()

        def all_sent(self):
            for at in range(28):
                self.copy(me, 0, pc, at).wait_send()

    cur = Gather(cur_buf, cur_send, cur_recv)
    hid = Gather(hid_buf, hid_send, hid_recv)
    beyond = flipped(diag, 1), flipped(px, 1), flipped(py, 1)
    cur.first(0)
    cur.second(0)
    par_sent, par_came = small_copies(par_buf, par_send, par_recv)
    for one in par_sent:
        one.start()
    cur.first(1)
    cur.second(1)

    def row(ref, layer):
        picked = ref[0:1]
        for at in range(1, layers):
            picked = jnp.where(layer == at, ref[at : at + 1], picked)
        return picked

    def one_layer(layer, carry):
        value_copy, gate_copy, out_copy = weight_copies(layer)
        value_copy.wait()
        gate_copy.wait()

        def consume_current(slot, first):
            at = pl.multiple_of(slot * local_width, LANES)
            block = cur_buf[slot].astype(jnp.float32)
            squared = block * block
            partial = squared[:, :LANES]
            for lane in range(LANES, local_width, LANES):
                partial = partial + squared[:, lane : lane + LANES]
            gained = (block * gain32[layer, :, pl.ds(at, local_width)]).astype(jnp.bfloat16)
            product = against(gained, weights[layer, :, pl.ds(at, local_width)])
            if first:
                squares[...] = partial
                acc[...] = product
            else:
                squares[...] += partial
                acc[...] += product

        consume_current(me, True)
        cur.relay_first(0)
        cur.half_arrived(pc, 0)
        cur.relay_first(1)
        cur.half_arrived(pc, 1)
        consume_current(pc, False)
        cur.relay_second(0)
        cur.relay_second(1)
        consume_current(px, False)
        consume_current(py, False)
        for slot in beyond[1:]:
            cur.half_arrived(slot, 0)
            cur.half_arrived(slot, 1)
            consume_current(slot, False)
        cur.relay_third(0)
        cur.relay_third(1)
        consume_current(diag, False)
        cur.half_arrived(beyond[0], 0)
        cur.half_arrived(beyond[0], 1)
        consume_current(beyond[0], False)

        scale = lax.rsqrt(jnp.sum(squares[...], axis=1, keepdims=True) / width + EPSILON)
        gated = (
            acc[:, :local_channels]
            * scale
            * jax.nn.sigmoid(acc[:, local_channels:] * scale)
        ).astype(jnp.bfloat16)
        gated_buf[...] = gated[rows - halo_rows :]

        def halo_copy(to):
            return pltpu.make_async_remote_copy(
                src_ref=gated_buf,
                dst_ref=halo.at[layer],
                send_sem=halo_send,
                recv_sem=halo_recv.at[layer],
                device_id=(to, me),
                device_id_type=MESH,
            )

        @pl.when(sp < sp_count - 1)
        def _():
            halo_copy(sp + 1).start()

        padded[pl.ds(halo_rows, rows)] = gated.astype(jnp.float32)

        @pl.when(sp == 0)
        def _():
            padded[pl.ds(0, halo_rows)] = jnp.zeros((halo_rows, local_channels), jnp.float32)

        tile = min(64, rows)
        bias = row(bias_ref, layer)

        def convolve(first_row):
            for lane in range(0, local_channels, LANES):
                total = jnp.broadcast_to(bias[:, lane : lane + LANES], (tile, LANES))
                for tap in range(taps):
                    total = total + kernel_ref[layer, tap : tap + 1, lane : lane + LANES] * padded[
                        first_row + skip + tap : first_row + skip + tap + tile, lane : lane + LANES
                    ]
                conv[first_row : first_row + tile, lane : lane + LANES] = total

        for first_row in range(tile, rows, tile):
            convolve(first_row)

        @pl.when(sp > 0)
        def _():
            halo_copy(sp - 1).wait_recv()
            padded[pl.ds(0, halo_rows)] = halo[layer].astype(jnp.float32)

        convolve(0)

        convolved = conv[...]
        hid_buf[me] = convolved.astype(jnp.bfloat16)
        hid.first(0)
        lanes = lax.broadcasted_iota(jnp.int32, (rows, LANES), 1)
        total = jnp.sum(convolved, axis=1, keepdims=True)
        total_squared = jnp.sum(convolved * convolved, axis=1, keepdims=True)
        both = jnp.where(lanes == 0, total, jnp.where(lanes == 1, total_squared, 0.0))
        stat_buf[me] = both.T[:SUBLANES]

        stat_sent, stat_came = small_copies(stat_buf, stat_send, stat_recv)
        for one in stat_sent:
            one.start()
        hid.second(0)
        hid.first(1)
        cur.all_sent()
        out_copy.wait()
        hid.relay_first(0)
        hid.second(1)
        hid.relay_first(1)
        for one in stat_came:
            one.wait_recv()
        summed = stat_buf[0]
        for slot in range(1, tp_count):
            summed = summed + stat_buf[slot]
        summed = jnp.concatenate(
            [summed, jnp.zeros((LANES - SUBLANES, rows), jnp.float32)], axis=0
        ).T
        centre = summed[:, 0:1] / channels
        spread = summed[:, 1:2] / channels - centre * centre
        steepness = lax.rsqrt(spread + EPSILON)

        def consume_hidden(slot, h, first):
            at = pl.multiple_of(slot * local_channels, LANES)
            here = slice(h * half, (h + 1) * half)
            gain = par_buf[slot, 0:1]
            shift = par_buf[slot, layers : layers + 1]
            for other in range(1, layers):
                gain = jnp.where(layer == other, par_buf[slot, other : other + 1], gain)
                shift = jnp.where(
                    layer == other, par_buf[slot, layers + other : layers + other + 1], shift
                )
            normal_out = (hid_buf[slot, here].astype(jnp.float32) - centre[here]) * steepness[
                here
            ] * gain + shift
            hidden = (normal_out / (1.0 + jnp.exp(-normal_out))).astype(jnp.bfloat16)
            product = jnp.dot(
                hidden,
                out_weights[layer, pl.ds(at, local_channels)],
                preferred_element_type=jnp.float32,
            )
            if first:
                acc[here, :local_width] = product
            else:
                acc[here, :local_width] += product

        def finish(h):
            for slot in beyond[1:]:
                hid.half_arrived(slot, h)
                consume_hidden(slot, h, False)
            consume_hidden(diag, h, False)
            hid.half_arrived(beyond[0], h)
            consume_hidden(beyond[0], h, False)
            here = slice(h * half, (h + 1) * half)
            cur_buf[me, here] = (
                cur_buf[me, here].astype(jnp.float32) + acc[here, :local_width]
            ).astype(jnp.bfloat16)

            @pl.when(layer < layers - 1)
            def _():
                cur.first(h)
                cur.second(h)

        @pl.when(layer == 0)
        def _():
            for one in par_came:
                one.wait_recv()
            for one in par_sent:
                one.wait_send()

        for h in range(2):
            if h == 1:
                hid.relay_third(1)
            consume_hidden(me, h, True)
            hid.half_arrived(pc, h)
            consume_hidden(pc, h, False)
            if h == 0:
                hid.relay_second(0)
                hid.relay_second(1)
            consume_hidden(px, h, False)
            consume_hidden(py, h, False)
            if h == 0:
                hid.relay_third(0)
            finish(h)
        for one in stat_sent:
            one.wait_send()
        hid.all_sent()

        @pl.when(sp < sp_count - 1)
        def _():
            halo_copy(sp + 1).wait_send()

        return carry

    lax.fori_loop(0, layers, one_layer, 0)
    result_ref[...] = cur_buf[me]


def fused(
    sp_count,
    tp_count,
    stream,
    norm_gain,
    value_weight,
    gate_weight,
    kernel,
    kernel_bias,
    chan_gain,
    chan_shift,
    out_weight,
):
    layers, taps, local_channels = kernel.shape
    rows, local_width = stream.shape
    halo_rows = -(-(taps - 1) // 16) * 16
    par_rows = -(-2 * layers // SUBLANES) * SUBLANES
    any_space = pl.BlockSpec(memory_space=pl.ANY)
    vmem = pl.BlockSpec(memory_space=pltpu.VMEM)
    dma = pltpu.SemaphoreType.DMA
    return pl.pallas_call(
        functools.partial(fused_kernel, sp_count, tp_count),
        out_shape=jax.ShapeDtypeStruct((rows, local_width), jnp.bfloat16),
        in_specs=[any_space, vmem, any_space, any_space, vmem, vmem, vmem, vmem, any_space],
        out_specs=vmem,
        scratch_shapes=[
            pltpu.VMEM((tp_count, rows, local_width), jnp.bfloat16),
            pltpu.VMEM((tp_count, rows, local_channels), jnp.bfloat16),
            pltpu.VMEM((layers, 2 * local_channels, local_width * tp_count), jnp.bfloat16),
            pltpu.VMEM((layers,) + out_weight.shape[1:], jnp.bfloat16),
            pltpu.VMEM((layers, 1, local_width * tp_count), jnp.float32),
            pltpu.VMEM((rows, max(2 * local_channels, local_width)), jnp.float32),
            pltpu.VMEM((rows, LANES), jnp.float32),
            pltpu.VMEM((halo_rows + rows, local_channels), jnp.float32),
            pltpu.VMEM((rows, local_channels), jnp.float32),
            pltpu.VMEM((halo_rows, local_channels), jnp.bfloat16),
            pltpu.VMEM((layers, halo_rows, local_channels), jnp.bfloat16),
            pltpu.VMEM((tp_count, SUBLANES, rows), jnp.float32),
            pltpu.VMEM((tp_count, par_rows, local_channels), jnp.float32),
            dma((tp_count, 4)),
            dma((28,)),
            dma((tp_count, 4)),
            dma((28,)),
            dma((tp_count,)),
            dma((tp_count,)),
            dma((tp_count,)),
            dma((tp_count,)),
            dma((layers,)),
            dma,
            dma((3, layers)),
            dma,
        ],
        compiler_params=pltpu.CompilerParams(
            collective_id=0, has_side_effects=True, vmem_limit_bytes=60 * 1024 * 1024
        ),
    )(
        stream,
        norm_gain,
        value_weight,
        gate_weight,
        kernel,
        kernel_bias,
        chan_gain,
        chan_shift,
        out_weight,
    )


def solution(mesh):
    cube = mesh.shape["tp"] == 2**3
    body = functools.partial(fused, mesh.shape["sp"], mesh.shape["tp"]) if cube else on_device
    return jax.shard_map(
        body,
        mesh=mesh,
        in_specs=(
            P("sp", "tp"),
            P(),
            P(None, "tp", None),
            P(None, "tp", None),
            P(None, None, "tp"),
            P(None, "tp"),
            P(None, "tp"),
            P(None, "tp"),
            P(None, None, "tp"),
        ),
        out_specs=P("sp", "tp"),
        check_vma=False,
    )
```
